32 devices in a mesh: sp: 16 (over z, y, x), tp: 2 (over core).
Axes of the slice: x: 2, y: 2, z: 4, core: 2. Of those that a mesh axis runs over, the one named last changes fastest.
Arguments:
- tokens: bfloat16 [2048, 2048], P('sp'), may hold values from -6 to 6
- norm_gain: float32 [2048], replicated, may hold values from 0.1 to 1.9
- conv_value_weight: bfloat16 [2048, 1024], P('sp', 'tp'), may hold values from -0.125 to 0.125
- conv_gate_weight: bfloat16 [2048, 1024], P('sp', 'tp'), may hold values from -0.125 to 0.125
- conv_kernel: float32 [31, 1024], P(None, 'tp'), may hold values from -10 to 10
- conv_bias: float32 [1024], P('tp'), may hold values from -4 to 4
- channel_gain: float32 [1024], P('tp'), may hold values from 0.1 to 1.9
- query_weight: bfloat16 [2048, 2048], P('sp', 'tp'), may hold values from -0.125 to 0.125
- key_weight: bfloat16 [2048, 2048], P('sp', 'tp'), may hold values from -0.125 to 0.125
- value_weight: bfloat16 [2048, 4096], P('sp', 'tp'), may hold values from -0.125 to 0.125
- gate_weight: bfloat16 [2048, 32], replicated, may hold values from -0.125 to 0.125
- gate_offset: float32 [2, 2, 8, 2048], P(None, None, 'tp', 'sp'), may hold values from -110 to 160, as said below
- start_memory: float32 [2, 8, 512, 256], P(None, 'tp'), may hold values from -0.375 to 0.375
- start_norm: float32 [2, 8, 256], P(None, 'tp'), may hold values from -0.375 to 0.375
- start_level: float32 [2, 8], P(None, 'tp'), may hold values from 2 to 5
- cell_gain: float32 [4096], P('tp'), may hold values from 0.1 to 1.9
- out_conv_weight: bfloat16 [2048, 1024], P('sp', 'tp'), may hold values from -0.25 to 0.25
- out_cell_weight: bfloat16 [2048, 4096], P('sp', 'tp'), may hold values from -0.09375 to 0.09375
Outputs:
- mixed: bfloat16 [2048, 2048], P(('sp', 'tp'))
The draws below stay inside these ranges and needn't reach their ends.
Inputs may be any that keep to these rules, and one draw needn't show every extreme that they name: `gate_offset`: added to the gate pre-activations; index 0 of the second dimension is the input gate, index 1 the forget gate.
All inputs are finite; a program needn't handle non-finite values.
Results may differ from the reference program's by a relative error of at most 0.017.
Values may be sent and summed in bfloat16 or wider, within the bound.
A program may use at most 192 MiB of HBM per device.

```python
import math
import jax
import jax.numpy as jnp
from jax import lax

D = 2048
CONV_W = 1024
MEMORY_GROUPS = 8
KEY_DIM = 256
VALUE_DIM = 512
KERNEL = 31
BLOCK = 128
TOK_DEV = 128
STEP_COUNT = 2048
N_TP = 2


def draw_conv_kernel(key, part):
    base_key, rough_key = jax.random.split(jax.random.fold_in(key, 11))
    channel = jnp.arange(CONV_W, dtype=jnp.float32) / CONV_W
    roughness = jnp.exp(jax.random.uniform(rough_key, (CONV_W,), minval=-0.5, maxval=0.5))
    channel_scale = jnp.exp(math.log(8.0) * channel)
    entries = jnp.clip(jax.random.normal(base_key, (KERNEL, CONV_W)), -4.0, 4.0)
    return (entries * channel_scale * roughness / math.sqrt(KERNEL)).astype(jnp.float32)


def draw_gate_offset(key, part):
    frequency_seed, permute_seed, surge_seed, feature_seed = jax.random.split(jax.random.fold_in(key, 23), 4)
    step_index = jnp.arange(STEP_COUNT)
    device_block = step_index // TOK_DEV
    device_count = STEP_COUNT // TOK_DEV
    device_rate = jnp.exp(jax.random.uniform(frequency_seed, (2, MEMORY_GROUPS, device_count), minval=math.log(0.4), maxval=math.log(2.5)))
    rate_here = jnp.take(device_rate, device_block, axis=2)
    order_keys = jax.random.split(permute_seed, 2)
    head_rank = jnp.stack([jax.random.permutation(order_keys[0], MEMORY_GROUPS), jax.random.permutation(order_keys[1], MEMORY_GROUPS)])
    fast_count = MEMORY_GROUPS // 2
    slow_level = jnp.log(2.0 * STEP_COUNT / rate_here)
    input_part = jnp.clip(jax.random.normal(feature_seed, (2, MEMORY_GROUPS, STEP_COUNT)), -4.0, 4.0)
    fast_head = (head_rank < fast_count)[:, :, None]
    surge_index = jax.random.randint(surge_seed, (2, MEMORY_GROUPS, 2), 0, STEP_COUNT)
    surge_flags = jnp.any(step_index[None, None, None, :] == surge_index[:, :, :, None], axis=2)
    decay_fraction = jnp.where(fast_head, 3.2, slow_level)
    decay_fraction = jnp.where(surge_flags, 0.5, decay_fraction)
    return jnp.stack([input_part, decay_fraction], axis=1).astype(jnp.float32)


def steps_of(stream_key, dims, pieces, smallest, largest):
    def one(dim, shards_of):
        heights = jax.random.uniform(jax.random.fold_in(jax.random.fold_in(stream_key, 6), dim), (shards_of,), jnp.float32, smallest / len(pieces), largest / len(pieces))
        return jnp.repeat(jnp.exp(heights), dims[dim] // shards_of).reshape((-1,) + (1,) * (len(dims) - dim - 1))

    gain = one(*pieces[0])
    for cut in pieces[1:]:
        gain = gain * one(*cut)
    return gain


def centred(stream_key, extent, scale, bound, cuts=(), kind=jnp.bfloat16):
    gain = steps_of(stream_key, extent, cuts, -0.22, 0.18) if cuts else 1.0
    values = jax.random.normal(stream_key, extent, jnp.float32) * scale * gain
    return jnp.minimum(jnp.maximum(values, -bound), bound).astype(kind)


def setup_inputs(seed: int = 0) -> dict:
    seeds = jax.random.split(jax.random.key(seed), 19)
    tokens = centred(seeds[0], (STEP_COUNT, D), 1.0, 6.0, ((0, 16),))
    norm_gain = jnp.clip(1.0 + 0.18 * jax.random.normal(seeds[1], (D,), jnp.float32), 0.1, 1.9)
    conv_value_weight = centred(seeds[2], (D, CONV_W), D ** -0.5, 0.125, ((0, 16), (1, 2)))
    conv_gate_weight = centred(seeds[3], (D, CONV_W), D ** -0.5, 0.125, ((0, 16), (1, 2)))
    conv_kernel = draw_conv_kernel(jax.random.fold_in(seeds[18], 71), 0)
    conv_bias = centred(seeds[5], (CONV_W,), 1.0, 4.0, ((0, 2),), jnp.float32)
    channel_gain = jnp.clip(1.0 + 0.18 * jax.random.normal(seeds[6], (CONV_W,), jnp.float32), 0.1, 1.9)
    query_weight = centred(seeds[7], (D, MEMORY_GROUPS * KEY_DIM), D ** -0.5, 0.125, ((0, 16), (1, 2)))
    key_weight = centred(seeds[8], (D, MEMORY_GROUPS * KEY_DIM), D ** -0.5, 0.125, ((0, 16), (1, 2)))
    value_weight = centred(seeds[9], (D, MEMORY_GROUPS * VALUE_DIM), D ** -0.5, 0.125, ((0, 16), (1, 2)))
    gate_weight = centred(seeds[10], (D, 4 * MEMORY_GROUPS), D ** -0.5, 0.125)
    gate_offset = draw_gate_offset(jax.random.fold_in(seeds[18], 71), 0)
    start_memory = centred(seeds[12], (2, MEMORY_GROUPS, VALUE_DIM, KEY_DIM), KEY_DIM ** -0.5, 0.375, ((1, 2),), jnp.float32)
    start_norm = centred(seeds[13], (2, MEMORY_GROUPS, KEY_DIM), KEY_DIM ** -0.5, 0.375, ((1, 2),), jnp.float32)
    start_level = jnp.clip(2.0 + 3.0 * jax.random.uniform(seeds[14], (2, MEMORY_GROUPS), jnp.float32) ** steps_of(seeds[14], (2, MEMORY_GROUPS), ((1, 2),), -0.2, 0.2), 2.0, 5.0)
    cell_gain = jnp.clip(1.0 + 0.18 * jax.random.normal(seeds[15], (MEMORY_GROUPS * VALUE_DIM,), jnp.float32), 0.1, 1.9)
    out_conv_weight = centred(seeds[16], (D, CONV_W), (CONV_W // 2) ** -0.5, 0.25, ((0, 16), (1, 2)))
    out_cell_weight = centred(seeds[17], (D, MEMORY_GROUPS * VALUE_DIM), (MEMORY_GROUPS * VALUE_DIM) ** -0.5, 0.09375, ((0, 16), (1, 2)))
    return {"tokens": tokens, "norm_gain": norm_gain, "conv_value_weight": conv_value_weight, "conv_gate_weight": conv_gate_weight, "conv_kernel": conv_kernel, "conv_bias": conv_bias, "channel_gain": channel_gain, "query_weight": query_weight, "key_weight": key_weight, "value_weight": value_weight, "gate_weight": gate_weight, "gate_offset": gate_offset, "start_memory": start_memory, "start_norm": start_norm, "start_level": start_level, "cell_gain": cell_gain, "out_conv_weight": out_conv_weight, "out_cell_weight": out_cell_weight}


EPS = 1e-06
HIGHEST = lax.Precision.HIGHEST

def back_to_wide(values):
    return lax.optimization_barrier(values.astype(jnp.bfloat16)).astype(jnp.float32)

def block_step(carried, inputs):
    memory, normer, run_level = carried
    queries, key_rows, value_rows, in_gate, log_forget = inputs
    length = queries.shape[0]
    lower_mask = jnp.arange(length)[:, None] >= jnp.arange(length)[None, :]
    cumulative = jnp.cumsum(log_forget)
    decay_table = jnp.where(lower_mask, cumulative[:, None] - cumulative[None, :] + in_gate[None, :], -jnp.inf)
    carried_level = cumulative + run_level
    top_level = jnp.maximum(carried_level, lax.optimization_barrier(jnp.max(decay_table, axis=1)))
    carry_weight = jnp.exp(carried_level - top_level)
    scores = jnp.dot(queries, key_rows.T, precision=HIGHEST) * jnp.exp(decay_table - top_level[:, None])
    numerator = jnp.dot(scores, value_rows, precision=HIGHEST) + carry_weight[:, None] * jnp.dot(queries, memory.T, precision=HIGHEST)
    denominator = lax.optimization_barrier(jnp.sum(scores, axis=1)) + carry_weight * jnp.dot(queries, normer, precision=HIGHEST)
    outputs = numerator / jnp.maximum(jnp.abs(denominator), 1.0)[:, None]
    block_total = cumulative[-1]
    tail_level = block_total - cumulative + in_gate
    new_level = jnp.maximum(block_total + run_level, jnp.max(tail_level))
    old_weight = jnp.exp(block_total + run_level - new_level)
    new_weight = jnp.exp(tail_level - new_level)
    memory = old_weight * memory + jnp.dot((value_rows * new_weight[:, None]).T, key_rows, precision=HIGHEST)
    normer = old_weight * normer + jnp.dot(new_weight, key_rows, precision=HIGHEST)
    return ((memory, normer, new_level), outputs)

def run_cell(queries, key_rows, value_rows, in_gate, log_forget, memory, normer, run_level):
    blocks = queries.shape[0] // BLOCK

    def to_blocks(values):
        return values.reshape((blocks, BLOCK) + values.shape[1:])
    final_state, outputs = lax.scan(block_step, (memory, normer, run_level), tuple((to_blocks(values) for values in (queries, key_rows, value_rows, in_gate, log_forget))))
    return outputs.reshape(queries.shape[0], value_rows.shape[1])

def head_outputs(inputs):
    queries, key_rows, value_rows, in_gate, log_forget, memory, normer, run_level = inputs
    forward = run_cell(queries, key_rows, value_rows, in_gate[0], log_forget[0], memory[0], normer[0], run_level[0])
    backward = run_cell(queries[::-1], key_rows[::-1], value_rows[::-1], in_gate[1, ::-1], log_forget[1, ::-1], memory[1], normer[1], run_level[1])[::-1]
    both_ways = forward + backward
    return both_ways * lax.rsqrt(lax.optimization_barrier(jnp.mean(both_ways * both_ways, axis=1, keepdims=True)) + EPS)

def reference(tokens, norm_gain, conv_value_weight, conv_gate_weight, conv_kernel, conv_bias, channel_gain, query_weight, key_weight, value_weight, gate_weight, gate_offset, start_memory, start_norm, start_level, cell_gain, out_conv_weight, out_cell_weight):
    features = tokens.astype(jnp.float32)
    normed = (features * lax.rsqrt(lax.optimization_barrier(jnp.mean(features * features, axis=1, keepdims=True)) + EPS) * norm_gain).astype(jnp.bfloat16)

    def project(weight):
        return jnp.dot(normed, weight, preferred_element_type=jnp.float32)
    conv_value = project(conv_value_weight).astype(jnp.bfloat16)
    conv_gate = project(conv_gate_weight).astype(jnp.bfloat16)
    gated_rows = (conv_value.astype(jnp.float32) * jax.nn.sigmoid(conv_gate.astype(jnp.float32))).astype(jnp.bfloat16)
    half_reach = KERNEL // 2
    padded = jnp.pad(gated_rows.astype(jnp.float32), ((half_reach, half_reach), (0, 0)))
    conv_sum = conv_bias + sum((conv_kernel[offset] * padded[offset:offset + STEP_COUNT] for offset in range(KERNEL)))
    channel_mean = lax.optimization_barrier(jnp.mean(conv_sum, axis=1, keepdims=True))
    channel_var = lax.optimization_barrier(jnp.mean(conv_sum * conv_sum, axis=1, keepdims=True)) - channel_mean * channel_mean
    conv_out = jax.nn.silu((conv_sum - channel_mean) * lax.rsqrt(channel_var + EPS) * channel_gain).astype(jnp.bfloat16)

    def split_heads(flat_rows, head_width):
        return jnp.transpose(back_to_wide(flat_rows).reshape(STEP_COUNT, MEMORY_GROUPS, head_width), (1, 0, 2))
    queries = split_heads(project(query_weight), KEY_DIM)
    key_rows = split_heads(project(key_weight), KEY_DIM) * KEY_DIM ** (-0.5)
    value_rows = split_heads(project(value_weight), VALUE_DIM)
    gate_pre = project(gate_weight).reshape(STEP_COUNT, 2, 2, MEMORY_GROUPS)
    gate_pre = jnp.transpose(gate_pre, (1, 2, 3, 0)) + gate_offset
    in_gate = jnp.transpose(gate_pre[:, 0], (1, 0, 2))
    log_forget = jnp.transpose(jax.nn.log_sigmoid(gate_pre[:, 1]), (1, 0, 2))
    cells = lax.map(head_outputs, (queries, key_rows, value_rows, in_gate, log_forget, jnp.transpose(start_memory, (1, 0, 2, 3)), jnp.transpose(start_norm, (1, 0, 2)), jnp.transpose(start_level, (1, 0))))
    cell_out = (jnp.transpose(cells, (1, 0, 2)).reshape(STEP_COUNT, MEMORY_GROUPS * VALUE_DIM) * cell_gain).astype(jnp.bfloat16)
    conv_groups = conv_out.reshape(STEP_COUNT, N_TP, CONV_W // N_TP)
    cell_groups = cell_out.reshape(STEP_COUNT, N_TP, MEMORY_GROUPS * VALUE_DIM // N_TP)
    conv_weights = out_conv_weight.reshape(D, N_TP, CONV_W // N_TP)
    cell_weights = out_cell_weight.reshape(D, N_TP, MEMORY_GROUPS * VALUE_DIM // N_TP)
    mixed_sum = jnp.zeros((STEP_COUNT, D), jnp.float32)
    for group in range(N_TP):
        partial_value = jnp.einsum('tc,dc->td', conv_groups[:, group], conv_weights[:, group], preferred_element_type=jnp.float32) + jnp.einsum('tc,dc->td', cell_groups[:, group], cell_weights[:, group], preferred_element_type=jnp.float32)
        mixed_sum = mixed_sum + lax.optimization_barrier(partial_value.astype(jnp.bfloat16)).astype(jnp.float32)
    return mixed_sum.astype(jnp.bfloat16)
```

```python
import jax
import jax.numpy as jnp
from jax import lax
from jax.sharding import Mesh, PartitionSpec as P

EPS = 1e-06
HIGHEST = lax.Precision.HIGHEST
CHUNK = 128
OUTER, HEAD, TP = "outer", "head", "tp"


def running_sum(values):
    lead, length = values.shape[:-1], values.shape[-1]
    chunk = min(CHUNK, length)
    count = length // chunk
    blocks = values.reshape(lead + (count, chunk))
    inside = (jnp.arange(chunk)[:, None] <= jnp.arange(chunk)[None, :]).astype(jnp.float32)
    before = (jnp.arange(count)[:, None] < jnp.arange(count)[None, :]).astype(jnp.float32)
    local = jnp.einsum("...cs,st->...ct", blocks, inside, precision=HIGHEST)
    start = jnp.einsum("...c,cd->...d", local[..., -1], before, precision=HIGHEST)
    return (local + start[..., None]).reshape(values.shape)


def own_columns(weight, parts, part):
    return lax.dynamic_slice_in_dim(
        weight, part * (weight.shape[-1] // parts), weight.shape[-1] // parts, weight.ndim - 1
    )


def by_head(weights, parts):
    return jnp.concatenate(
        [
            jnp.transpose(w.reshape(w.shape[0], parts, w.shape[1] // parts), (1, 0, 2))
            for w in weights
        ],
        axis=2,
    )


def spread(blocks):
    mine = lax.all_to_all(blocks, HEAD, 0, 0, tiled=True)
    return mine.reshape(mine.shape[0] * mine.shape[1], mine.shape[2])


def shards(
    tokens,
    norm_gain,
    conv_value_weight,
    conv_gate_weight,
    conv_kernel,
    conv_bias,
    channel_gain,
    query_weight,
    key_weight,
    value_weight,
    gate_weight,
    gate_offset,
    start_memory,
    start_norm,
    start_level,
    cell_gain,
    out_conv_weight,
    out_cell_weight,
):
    parts = lax.axis_size(HEAD)
    groups = lax.axis_size(OUTER)
    group = lax.axis_index(OUTER)
    part = lax.axis_index(HEAD)
    key_width = start_norm.shape[2]
    value_width = start_memory.shape[2]
    all_channels = conv_bias.shape[0] * lax.axis_size(TP)
    heads_here = start_level.shape[1]
    channels = conv_bias.shape[0] // parts

    features = tokens.astype(jnp.float32)
    normed = (
        features * lax.rsqrt(jnp.mean(features * features, axis=1, keepdims=True) + EPS) * norm_gain
    ).astype(jnp.bfloat16)

    gate_pre = jnp.dot(normed, gate_weight, preferred_element_type=jnp.float32)
    gate_pre = gate_pre.reshape(gate_pre.shape[0], 2, 2, gate_weight.shape[1] // 4)
    gate_pre = lax.dynamic_slice_in_dim(gate_pre, lax.axis_index(TP) * heads_here, heads_here, 3)
    gate_pre = jnp.transpose(gate_pre, (1, 2, 3, 0)) + gate_offset
    gates = lax.all_gather(gate_pre, (OUTER, HEAD), axis=3, tiled=True)
    gates = lax.dynamic_index_in_dim(gates, part, 2, False)

    rows = lax.all_gather(normed, HEAD, axis=0, tiled=True)
    here = rows.shape[0]

    key_value_part = lax.all_gather(
        spread(by_head((key_weight, value_weight), parts)), OUTER, axis=0, tiled=True
    )
    other_part = lax.all_gather(
        spread(by_head((conv_value_weight, conv_gate_weight, query_weight), parts)),
        OUTER,
        axis=0,
        tiled=True,
    )
    out_part = lax.all_gather(
        spread(by_head((out_conv_weight, out_cell_weight), parts)), OUTER, axis=0, tiled=True
    )

    key_value = jnp.dot(rows, key_value_part, preferred_element_type=jnp.float32).astype(
        jnp.bfloat16
    )
    all_key_value = lax.all_gather(key_value, OUTER, axis=0, tiled=True)

    others = jnp.dot(rows, other_part, preferred_element_type=jnp.float32).astype(jnp.bfloat16)
    queries = others[:, 2 * channels :]

    gated = (
        others[:, :channels].astype(jnp.float32)
        * jax.nn.sigmoid(others[:, channels : 2 * channels].astype(jnp.float32))
    ).astype(jnp.bfloat16)
    reach = conv_kernel.shape[0] // 2
    up = [(i, i + 1) for i in range(groups - 1)]
    down = [(j, i) for i, j in up]
    before = lax.ppermute(gated[here - reach :], OUTER, up)
    after = lax.ppermute(gated[:reach], OUTER, down)
    padded = jnp.concatenate([before, gated, after], axis=0).astype(jnp.float32)
    taps = own_columns(conv_kernel, parts, part)
    conv_sum = own_columns(conv_bias, parts, part) + sum(
        taps[offset] * padded[offset : offset + here] for offset in range(conv_kernel.shape[0])
    )
    stats = lax.psum(
        jnp.stack([jnp.sum(conv_sum, axis=1), jnp.sum(conv_sum * conv_sum, axis=1)]), (HEAD, TP)
    )
    channel_mean = stats[0] / all_channels
    channel_var = stats[1] / all_channels - channel_mean * channel_mean
    conv_out = jax.nn.silu(
        (conv_sum - channel_mean[:, None])
        * lax.rsqrt(channel_var + EPS)[:, None]
        * own_columns(channel_gain, parts, part)
    ).astype(jnp.bfloat16)

    total = gates.shape[2]
    in_gate = gates[:, 0]
    log_forget = jax.nn.log_sigmoid(gates[:, 1])
    whole = jnp.round(log_forget)
    both = jnp.stack([whole, log_forget - whole])
    both = jnp.stack([both[:, 0], jnp.flip(both[:, 1], axis=1)], axis=1)
    both = running_sum(both)
    passed = jnp.stack([both[:, 0], jnp.flip(both[:, 1], axis=1)], axis=1)
    passed_here = lax.dynamic_slice_in_dim(passed, group * here, here, 2)
    keys = all_key_value[:, :key_width]
    values = all_key_value[:, key_width:]
    products = lax.dot_general(
        queries, keys, (((1,), (1,)), ((), ())), preferred_element_type=jnp.float32
    ) * (key_width**-0.5)
    at_row = (group * here + jnp.arange(here))[:, None]
    at_column = jnp.arange(total)[None, :]
    levels = lax.dynamic_index_in_dim(start_level, part, 1, False)
    norms = lax.dynamic_index_in_dim(start_norm, part, 1, False)
    memories = lax.dynamic_index_in_dim(start_memory, part, 1, False)
    wide_queries = queries.astype(jnp.float32)
    scaled = 0.0
    entered = 0.0
    for way in range(2):
        row_whole, row_rest = passed_here[0, way], passed_here[1, way]
        table = (row_whole[:, None] - passed[0, way][None, :]) + (
            row_rest[:, None] + (in_gate[way] - passed[1, way])[None, :]
        )
        seen = at_column <= at_row if way == 0 else at_column >= at_row
        table = jnp.where(seen, table, -jnp.inf)
        start = row_whole + row_rest + levels[way]
        top = jnp.maximum(start, jnp.max(table, axis=1))
        scores = products * jnp.exp(table - top[:, None])
        entry = jnp.exp(start - top)
        denominator = jnp.sum(scores, axis=1) + entry * jnp.sum(
            wide_queries * norms[way][None, :], axis=1
        )
        inverse = 1.0 / jnp.maximum(jnp.abs(denominator), 1.0)
        scaled = scaled + scores * inverse[:, None]
        entered = entered + (entry * inverse)[:, None] * lax.dot_general(
            queries,
            memories[way].astype(jnp.bfloat16),
            (((1,), (1,)), ((), ())),
            preferred_element_type=jnp.float32,
        )
    both_ways = entered + jnp.dot(
        scaled.astype(jnp.bfloat16), values, preferred_element_type=jnp.float32
    )
    both_ways = both_ways * lax.rsqrt(jnp.mean(both_ways * both_ways, axis=1, keepdims=True) + EPS)
    cell_out = (both_ways * own_columns(cell_gain, parts, part)).astype(jnp.bfloat16)

    partial = lax.dot_general(
        jnp.concatenate([conv_out, cell_out], axis=1),
        out_part,
        (((1,), (1,)), ((), ())),
        preferred_element_type=jnp.float32,
    ).astype(jnp.bfloat16)
    return lax.psum_scatter(partial, (HEAD, TP), scatter_dimension=0, tiled=True)


def solution(mesh):
    split = (OUTER, HEAD)
    in_specs = (
        P(split, None),
        P(),
        P(split, TP),
        P(split, TP),
        P(None, TP),
        P(TP),
        P(TP),
        P(split, TP),
        P(split, TP),
        P(split, TP),
        P(),
        P(None, None, TP, split),
        P(None, TP, None, None),
        P(None, TP, None),
        P(None, TP),
        P(TP),
        P(split, TP),
        P(split, TP),
    )
    out_specs = P((OUTER, HEAD, TP), None)

    def run(*arrays):
        sequence, tensor = mesh.shape["sp"], mesh.shape["tp"]
        heads = arrays[14].shape[1] // tensor
        parts = heads if sequence % heads == 0 else 1
        assert parts == heads
        fine = Mesh(mesh.devices.reshape(sequence // parts, parts, tensor), (OUTER, HEAD, TP))
        return jax.shard_map(
            shards, mesh=fine, in_specs=in_specs, out_specs=out_specs, check_vma=False
        )(*arrays)

    return run
```

```python
import functools

import jax
import jax.numpy as jnp
from jax import lax
from jax.experimental import pallas as pl
from jax.experimental.pallas import tpu as pltpu
from jax.sharding import Mesh, PartitionSpec as P

EPS = 1e-06
HIGHEST = lax.Precision.HIGHEST
CHUNK = 128
OUTER, HEAD, TP = "outer", "head", "tp"


def running_sum(values):
    lead, length = values.shape[:-1], values.shape[-1]
    chunk = min(CHUNK, length)
    count = length // chunk
    blocks = values.reshape(lead + (count, chunk))
    inside = (jnp.arange(chunk)[:, None] <= jnp.arange(chunk)[None, :]).astype(jnp.float32)
    before = (jnp.arange(count)[:, None] < jnp.arange(count)[None, :]).astype(jnp.float32)
    local = jnp.einsum("...cs,st->...ct", blocks, inside, precision=HIGHEST)
    start = jnp.einsum("...c,cd->...d", local[..., -1], before, precision=HIGHEST)
    return (local + start[..., None]).reshape(values.shape)


def own_columns(weight, parts, part):
    return lax.dynamic_slice_in_dim(
        weight, part * (weight.shape[-1] // parts), weight.shape[-1] // parts, weight.ndim - 1
    )


def by_head(weights, parts):
    return jnp.concatenate(
        [
            jnp.transpose(w.reshape(w.shape[0], parts, w.shape[1] // parts), (1, 0, 2))
            for w in weights
        ],
        axis=2,
    )


def spread(blocks):
    mine = lax.all_to_all(blocks, HEAD, 0, 0, tiled=True)
    return mine.reshape(mine.shape[0] * mine.shape[1], mine.shape[2])


MESH = pl.DeviceIdType.MESH


def exchange_kernel(groups, parts, *refs):
    normed, gates, key, value, conv_value, conv_gate, query, out_conv, out_cell = refs[:9]
    rows, all_gates, key_value, others, outs = refs[9:14]
    send, recv, local = refs[14:]
    group, part = lax.axis_index(OUTER), lax.axis_index(HEAD)
    depth = key.shape[0]
    away = [(g, p) for g in range(groups) for p in range(parts) if (g, p) != (0, 0)]

    def device(step):
        return {
            OUTER: lax.rem(group + step[0], groups),
            HEAD: lax.rem(part + step[1], parts),
        }

    barrier = pltpu.get_barrier_semaphore()
    for step in away:
        pl.semaphore_signal(barrier, inc=1, device_id=device(step), device_id_type=MESH)
    pl.semaphore_wait(barrier, len(away))

    place = group * parts + part
    deep = pl.ds(pl.multiple_of(place * depth, depth), depth)
    flat = pl.ds(pl.multiple_of(part * depth, depth), depth)

    def pieces(target, step, stage):
        def columns(ref):
            width = ref.shape[1] // parts
            return ref.at[:, pl.ds(pl.multiple_of(target * width, width), width)]

        def packed(refs_in, ref_out, at):
            column = 0
            found = []
            for ref in refs_in:
                width = ref.shape[1] // parts
                found.append((columns(ref), ref_out.at[at, pl.ds(column, width)]))
                column += width
            return found

        if stage == 0:
            return [(normed, rows.at[flat])] if step[0] == 0 else []
        if stage == 1:
            return packed((key, value), key_value, deep) + [(gates, all_gates.at[place])]
        if stage == 2:
            return packed((conv_value, conv_gate, query), others, deep)
        return packed((out_conv, out_cell), outs, flat) if step[0] == 0 else []

    copies = []
    kept = []
    for stage in range(4):
        for step in away:
            for source, target in pieces(lax.rem(part + step[1], parts), step, stage):
                copies.append(
                    pltpu.make_async_remote_copy(
                        src_ref=source,
                        dst_ref=target,
                        send_sem=send.at[len(copies)],
                        recv_sem=recv.at[len(copies)],
                        device_id=device(step),
                        device_id_type=MESH,
                    )
                )
                copies[-1].start()
        for source, target in pieces(part, (0, 0), stage):
            kept.append(pltpu.make_async_copy(source, target, local.at[len(kept)]))
            kept[-1].start()
    for copy in kept:
        copy.wait()
    for copy in copies:
        copy.wait()


def exchange(groups, parts, *arrays):
    normed, gates, key, value, conv_value, conv_gate, query, out_conv, out_cell = arrays
    depth, count = key.shape[0], groups * parts

    def made(height, *weights):
        width = sum(w.shape[1] // parts for w in weights)
        return jax.ShapeDtypeStruct((height, width), key.dtype)

    shapes = (
        jax.ShapeDtypeStruct((parts * normed.shape[0], normed.shape[1]), normed.dtype),
        jax.ShapeDtypeStruct((count,) + gates.shape, gates.dtype),
        made(count * depth, key, value),
        made(count * depth, conv_value, conv_gate, query),
        made(parts * depth, out_conv, out_cell),
    )
    many = 6 * (count - 1) + 3 * (parts - 1)
    return pl.pallas_call(
        functools.partial(exchange_kernel, groups, parts),
        out_shape=shapes,
        in_specs=[pl.BlockSpec(memory_space=pltpu.VMEM)] * len(arrays),
        out_specs=[pl.BlockSpec(memory_space=pl.ANY)] * len(shapes),
        scratch_shapes=[
            pltpu.SemaphoreType.DMA((many,)),
            pltpu.SemaphoreType.DMA((many,)),
            pltpu.SemaphoreType.DMA((9,)),
        ],
        compiler_params=pltpu.CompilerParams(collective_id=1, has_side_effects=True),
        name="exchange",
    )(*arrays)


def scatter_kernel(parts, partial, out, met, sums, landed, send, recv, far_send, far_recv):
    part, side = lax.axis_index(HEAD), lax.axis_index(TP)
    other = 1 - side

    def peer(step):
        return {HEAD: lax.rem(part + step, parts)}

    barrier = pltpu.get_barrier_semaphore()
    pl.semaphore_signal(barrier, inc=1, device_id={TP: other}, device_id_type=MESH)
    for step in range(1, parts):
        pl.semaphore_signal(barrier, inc=1, device_id=peer(step), device_id_type=MESH)
    pl.semaphore_wait(barrier, parts)

    near = []
    order = list(range(1, parts)) + [0]
    for step in order:
        near.append(
            pltpu.make_async_remote_copy(
                src_ref=partial.at[lax.rem(part + step, parts), other],
                dst_ref=met.at[step],
                send_sem=send.at[step],
                recv_sem=recv.at[step],
                device_id={TP: other},
                device_id_type=MESH,
            )
        )
        near[-1].start()
    far = []
    for step, copy in zip(order, near):
        copy.wait()
        total = partial[lax.rem(part + step, parts), side].astype(jnp.float32) + met[step].astype(
            jnp.float32
        )
        sums[step] = total.astype(sums.dtype)
        if step:
            far.append(
                pltpu.make_async_remote_copy(
                    src_ref=sums.at[step],
                    dst_ref=landed.at[step],
                    send_sem=far_send.at[step],
                    recv_sem=far_recv.at[step],
                    device_id=peer(step),
                    device_id_type=MESH,
                )
            )
            far[-1].start()
    total = sums[0].astype(jnp.float32)
    for step, copy in zip(order, far):
        copy.wait()
        total = total + landed[step].astype(jnp.float32)
    out[...] = total.astype(out.dtype)


def scatter(parts, partial):
    sides = 2
    height, width = partial.shape[0] // (parts * sides), partial.shape[1]
    blocks = partial.reshape(parts, sides, height, width)
    stack = pltpu.VMEM((parts, height, width), partial.dtype)
    return pl.pallas_call(
        functools.partial(scatter_kernel, parts),
        out_shape=jax.ShapeDtypeStruct((height, width), partial.dtype),
        in_specs=[pl.BlockSpec(memory_space=pltpu.VMEM)],
        out_specs=pl.BlockSpec(memory_space=pltpu.VMEM),
        scratch_shapes=[stack, stack, stack] + [pltpu.SemaphoreType.DMA((parts,))] * 4,
        compiler_params=pltpu.CompilerParams(collective_id=2, has_side_effects=True),
        name="scatter",
    )(blocks)


def shards(
    tokens,
    norm_gain,
    conv_value_weight,
    conv_gate_weight,
    conv_kernel,
    conv_bias,
    channel_gain,
    query_weight,
    key_weight,
    value_weight,
    gate_weight,
    gate_offset,
    start_memory,
    start_norm,
    start_level,
    cell_gain,
    out_conv_weight,
    out_cell_weight,
):
    parts = lax.axis_size(HEAD)
    groups = lax.axis_size(OUTER)
    group = lax.axis_index(OUTER)
    part = lax.axis_index(HEAD)
    key_width = start_norm.shape[2]
    value_width = start_memory.shape[2]
    all_channels = conv_bias.shape[0] * lax.axis_size(TP)
    heads_here = start_level.shape[1]
    channels = conv_bias.shape[0] // parts

    features = tokens.astype(jnp.float32)
    normed = (
        features * lax.rsqrt(jnp.mean(features * features, axis=1, keepdims=True) + EPS) * norm_gain
    ).astype(jnp.bfloat16)

    gate_pre = jnp.dot(normed, gate_weight, preferred_element_type=jnp.float32)
    gate_pre = gate_pre.reshape(gate_pre.shape[0], 2, 2, gate_weight.shape[1] // 4)
    gate_pre = lax.dynamic_slice_in_dim(gate_pre, lax.axis_index(TP) * heads_here, heads_here, 3)
    gate_pre = jnp.transpose(gate_pre, (1, 2, 3, 0)) + gate_offset
    direct = 1 < parts and groups * parts <= 16
    if direct:
        rows, gates, key_value_part, other_part, out_rows = exchange(
            groups,
            parts,
            normed,
            gate_pre,
            key_weight,
            value_weight,
            conv_value_weight,
            conv_gate_weight,
            query_weight,
            out_conv_weight,
            out_cell_weight,
        )
        gates = lax.dynamic_index_in_dim(gates, part, 3, False)
        gates = jnp.transpose(gates, (1, 2, 0, 3)).reshape(gates.shape[1:3] + (-1,))
    else:
        gates = lax.all_gather(gate_pre, (OUTER, HEAD), axis=3, tiled=True)
        gates = lax.dynamic_index_in_dim(gates, part, 2, False)
        rows = lax.all_gather(normed, HEAD, axis=0, tiled=True)
        key_value_part = lax.all_gather(
            spread(by_head((key_weight, value_weight), parts)), OUTER, axis=0, tiled=True
        )
        other_part = lax.all_gather(
            spread(by_head((conv_value_weight, conv_gate_weight, query_weight), parts)),
            OUTER,
            axis=0,
            tiled=True,
        )
        out_rows = spread(by_head((out_conv_weight, out_cell_weight), parts))
    here = rows.shape[0]
    out_part = lax.all_gather(out_rows, OUTER, axis=0, tiled=True)

    key_value = jnp.dot(rows, key_value_part, preferred_element_type=jnp.float32).astype(
        jnp.bfloat16
    )
    if direct:
        around = [key_value] + [
            lax.ppermute(key_value, OUTER, [(i, (i + g) % groups) for i in range(groups)])
            for g in range(1, groups)
        ]
        sources = [lax.rem(group + groups - g, groups) for g in range(groups)]
        all_key_value = jnp.concatenate(around, axis=0)
    else:
        all_key_value = lax.all_gather(key_value, OUTER, axis=0, tiled=True)

    others = jnp.dot(rows, other_part, preferred_element_type=jnp.float32).astype(jnp.bfloat16)
    queries = others[:, 2 * channels :]

    gated = (
        others[:, :channels].astype(jnp.float32)
        * jax.nn.sigmoid(others[:, channels : 2 * channels].astype(jnp.float32))
    ).astype(jnp.bfloat16)
    reach = conv_kernel.shape[0] // 2
    up = [(i, i + 1) for i in range(groups - 1)]
    down = [(j, i) for i, j in up]
    before = lax.ppermute(gated[here - reach :], OUTER, up)
    after = lax.ppermute(gated[:reach], OUTER, down)
    padded = jnp.concatenate([before, gated, after], axis=0).astype(jnp.float32)
    taps = own_columns(conv_kernel, parts, part)
    conv_sum = own_columns(conv_bias, parts, part) + sum(
        taps[offset] * padded[offset : offset + here] for offset in range(conv_kernel.shape[0])
    )
    stats = lax.psum(
        jnp.stack([jnp.sum(conv_sum, axis=1), jnp.sum(conv_sum * conv_sum, axis=1)]), (HEAD, TP)
    )
    channel_mean = stats[0] / all_channels
    channel_var = stats[1] / all_channels - channel_mean * channel_mean
    conv_out = jax.nn.silu(
        (conv_sum - channel_mean[:, None])
        * lax.rsqrt(channel_var + EPS)[:, None]
        * own_columns(channel_gain, parts, part)
    ).astype(jnp.bfloat16)

    total = gates.shape[2]
    in_gate = gates[:, 0]
    log_forget = jax.nn.log_sigmoid(gates[:, 1])
    whole = jnp.round(log_forget)
    both = jnp.stack([whole, log_forget - whole])
    both = jnp.stack([both[:, 0], jnp.flip(both[:, 1], axis=1)], axis=1)
    both = running_sum(both)
    passed = jnp.stack([both[:, 0], jnp.flip(both[:, 1], axis=1)], axis=1)
    passed_here = lax.dynamic_slice_in_dim(passed, group * here, here, 2)
    at_column = jnp.arange(total)
    if direct:

        def around_ring(array):
            return jnp.concatenate(
                [lax.dynamic_slice_in_dim(array, g * here, here, array.ndim - 1) for g in sources],
                axis=-1,
            )

        at_column, in_gate, passed = (around_ring(a) for a in (at_column, in_gate, passed))
    at_column = at_column[None, :]
    keys = all_key_value[:, :key_width]
    values = all_key_value[:, key_width:]
    products = lax.dot_general(
        queries, keys, (((1,), (1,)), ((), ())), preferred_element_type=jnp.float32
    ) * (key_width**-0.5)
    at_row = (group * here + jnp.arange(here))[:, None]
    levels = lax.dynamic_index_in_dim(start_level, part, 1, False)
    norms = lax.dynamic_index_in_dim(start_norm, part, 1, False)
    memories = lax.dynamic_index_in_dim(start_memory, part, 1, False)
    wide_queries = queries.astype(jnp.float32)
    scaled = 0.0
    entered = 0.0
    for way in range(2):
        row_whole, row_rest = passed_here[0, way], passed_here[1, way]
        table = (row_whole[:, None] - passed[0, way][None, :]) + (
            row_rest[:, None] + (in_gate[way] - passed[1, way])[None, :]
        )
        seen = at_column <= at_row if way == 0 else at_column >= at_row
        table = jnp.where(seen, table, -jnp.inf)
        start = row_whole + row_rest + levels[way]
        top = jnp.maximum(start, jnp.max(table, axis=1))
        scores = products * jnp.exp(table - top[:, None])
        entry = jnp.exp(start - top)
        denominator = jnp.sum(scores, axis=1) + entry * jnp.sum(
            wide_queries * norms[way][None, :], axis=1
        )
        inverse = 1.0 / jnp.maximum(jnp.abs(denominator), 1.0)
        scaled = scaled + scores * inverse[:, None]
        entered = entered + (entry * inverse)[:, None] * lax.dot_general(
            queries,
            memories[way].astype(jnp.bfloat16),
            (((1,), (1,)), ((), ())),
            preferred_element_type=jnp.float32,
        )
    both_ways = entered + jnp.dot(
        scaled.astype(jnp.bfloat16), values, preferred_element_type=jnp.float32
    )
    both_ways = both_ways * lax.rsqrt(jnp.mean(both_ways * both_ways, axis=1, keepdims=True) + EPS)
    cell_out = (both_ways * own_columns(cell_gain, parts, part)).astype(jnp.bfloat16)

    partial = lax.dot_general(
        jnp.concatenate([conv_out, cell_out], axis=1),
        out_part,
        (((1,), (1,)), ((), ())),
        preferred_element_type=jnp.float32,
    ).astype(jnp.bfloat16)
    if direct and lax.axis_size(TP) == 2:
        return scatter(parts, partial)
    return lax.psum_scatter(partial, (HEAD, TP), scatter_dimension=0, tiled=True)


def solution(mesh):
    split = (OUTER, HEAD)
    in_specs = (
        P(split, None),
        P(),
        P(split, TP),
        P(split, TP),
        P(None, TP),
        P(TP),
        P(TP),
        P(split, TP),
        P(split, TP),
        P(split, TP),
        P(),
        P(None, None, TP, split),
        P(None, TP, None, None),
        P(None, TP, None),
        P(None, TP),
        P(TP),
        P(split, TP),
        P(split, TP),
    )
    out_specs = P((OUTER, HEAD, TP), None)

    def run(*arrays):
        sequence, tensor = mesh.shape["sp"], mesh.shape["tp"]
        heads = arrays[14].shape[1] // tensor
        parts = heads if sequence % heads == 0 else 1
        assert parts == heads
        fine = Mesh(mesh.devices.reshape(sequence // parts, parts, tensor), (OUTER, HEAD, TP))
        return jax.shard_map(
            shards, mesh=fine, in_specs=in_specs, out_specs=out_specs, check_vma=False
        )(*arrays)

    return run
```

```python
import functools

import jax
import jax.numpy as jnp
from jax import lax
from jax.experimental import pallas as pl
from jax.experimental.pallas import tpu as pltpu
from jax.sharding import Mesh, PartitionSpec as P

EPS = 1e-06
HIGHEST = lax.Precision.HIGHEST
CHUNK = 128
OUTER, HEAD, TP = "outer", "head", "tp"


def running_sum(values):
    lead, length = values.shape[:-1], values.shape[-1]
    chunk = min(CHUNK, length)
    count = length // chunk
    blocks = values.reshape(lead + (count, chunk))
    inside = (jnp.arange(chunk)[:, None] <= jnp.arange(chunk)[None, :]).astype(jnp.float32)
    before = (jnp.arange(count)[:, None] < jnp.arange(count)[None, :]).astype(jnp.float32)
    local = jnp.einsum("...cs,st->...ct", blocks, inside, precision=HIGHEST)
    start = jnp.einsum("...c,cd->...d", local[..., -1], before, precision=HIGHEST)
    return (local + start[..., None]).reshape(values.shape)


def own_columns(weight, parts, part):
    return lax.dynamic_slice_in_dim(
        weight, part * (weight.shape[-1] // parts), weight.shape[-1] // parts, weight.ndim - 1
    )


def by_head(weights, parts):
    return jnp.concatenate(
        [
            jnp.transpose(w.reshape(w.shape[0], parts, w.shape[1] // parts), (1, 0, 2))
            for w in weights
        ],
        axis=2,
    )


def spread(blocks):
    mine = lax.all_to_all(blocks, HEAD, 0, 0, tiled=True)
    return mine.reshape(mine.shape[0] * mine.shape[1], mine.shape[2])


MESH = pl.DeviceIdType.MESH


def exchange_kernel(groups, parts, *refs):
    normed, gates, key, value, conv_value, conv_gate, query, out_conv, out_cell = refs[:9]
    rows, all_gates, key_value, others, outs = refs[9:14]
    send, recv, local = refs[14:]
    group, part = lax.axis_index(OUTER), lax.axis_index(HEAD)
    depth = key.shape[0]
    away = [(g, p) for g in range(groups) for p in range(parts) if (g, p) != (0, 0)]

    def device(step):
        return {
            OUTER: lax.rem(group + step[0], groups),
            HEAD: lax.rem(part + step[1], parts),
        }

    barrier = pltpu.get_barrier_semaphore()
    for step in away:
        pl.semaphore_signal(barrier, inc=1, device_id=device(step), device_id_type=MESH)
    pl.semaphore_wait(barrier, len(away))

    place = group * parts + part
    deep = pl.ds(pl.multiple_of(place * depth, depth), depth)
    flat = pl.ds(pl.multiple_of(part * depth, depth), depth)

    def pieces(target, step, stage):
        def columns(ref):
            width = ref.shape[1] // parts
            return ref.at[:, pl.ds(pl.multiple_of(target * width, width), width)]

        def packed(refs_in, ref_out, at):
            column = 0
            found = []
            for ref in refs_in:
                width = ref.shape[1] // parts
                found.append((columns(ref), ref_out.at[at, pl.ds(column, width)]))
                column += width
            return found

        if stage == 0:
            return [(normed, rows.at[flat])] if step[0] == 0 else []
        if stage == 1:
            return packed((key, value), key_value, deep) + [(gates, all_gates.at[place])]
        if stage == 2:
            return packed((conv_value, conv_gate, query), others, deep)
        return packed((out_conv, out_cell), outs, flat) if step[0] == 0 else []

    copies = []
    kept = []
    for stage in range(4):
        for step in away:
            for source, target in pieces(lax.rem(part + step[1], parts), step, stage):
                copies.append(
                    pltpu.make_async_remote_copy(
                        src_ref=source,
                        dst_ref=target,
                        send_sem=send.at[len(copies)],
                        recv_sem=recv.at[len(copies)],
                        device_id=device(step),
                        device_id_type=MESH,
                    )
                )
                copies[-1].start()
        for source, target in pieces(part, (0, 0), stage):
            kept.append(pltpu.make_async_copy(source, target, local.at[len(kept)]))
            kept[-1].start()
    for copy in kept:
        copy.wait()
    for copy in copies:
        copy.wait()


def exchange(groups, parts, *arrays):
    normed, gates, key, value, conv_value, conv_gate, query, out_conv, out_cell = arrays
    depth, count = key.shape[0], groups * parts

    def made(height, *weights):
        width = sum(w.shape[1] // parts for w in weights)
        return jax.ShapeDtypeStruct((height, width), key.dtype)

    shapes = (
        jax.ShapeDtypeStruct((parts * normed.shape[0], normed.shape[1]), normed.dtype),
        jax.ShapeDtypeStruct((count,) + gates.shape, gates.dtype),
        made(count * depth, key, value),
        made(count * depth, conv_value, conv_gate, query),
        made(parts * depth, out_conv, out_cell),
    )
    many = 6 * (count - 1) + 3 * (parts - 1)
    return pl.pallas_call(
        functools.partial(exchange_kernel, groups, parts),
        out_shape=shapes,
        in_specs=[pl.BlockSpec(memory_space=pltpu.VMEM)] * len(arrays),
        out_specs=[pl.BlockSpec(memory_space=pl.ANY)] * len(shapes),
        scratch_shapes=[
            pltpu.SemaphoreType.DMA((many,)),
            pltpu.SemaphoreType.DMA((many,)),
            pltpu.SemaphoreType.DMA((9,)),
        ],
        compiler_params=pltpu.CompilerParams(collective_id=1, has_side_effects=True),
        name="exchange",
    )(*arrays)


def scatter_kernel(parts, partial, out, met, sums, landed, send, recv, far_send, far_recv):
    part, side = lax.axis_index(HEAD), lax.axis_index(TP)
    other = 1 - side

    def peer(step):
        return {HEAD: lax.rem(part + step, parts)}

    barrier = pltpu.get_barrier_semaphore()
    pl.semaphore_signal(barrier, inc=1, device_id={TP: other}, device_id_type=MESH)
    for step in range(1, parts):
        pl.semaphore_signal(barrier, inc=1, device_id=peer(step), device_id_type=MESH)
    pl.semaphore_wait(barrier, parts)

    near = []
    order = list(range(1, parts)) + [0]
    for step in order:
        near.append(
            pltpu.make_async_remote_copy(
                src_ref=partial.at[lax.rem(part + step, parts), other],
                dst_ref=met.at[step],
                send_sem=send.at[step],
                recv_sem=recv.at[step],
                device_id={TP: other},
                device_id_type=MESH,
            )
        )
        near[-1].start()
    far = []
    for step, copy in zip(order, near):
        copy.wait()
        total = partial[lax.rem(part + step, parts), side].astype(jnp.float32) + met[step].astype(
            jnp.float32
        )
        sums[step] = total.astype(sums.dtype)
        if step:
            far.append(
                pltpu.make_async_remote_copy(
                    src_ref=sums.at[step],
                    dst_ref=landed.at[step],
                    send_sem=far_send.at[step],
                    recv_sem=far_recv.at[step],
                    device_id=peer(step),
                    device_id_type=MESH,
                )
            )
            far[-1].start()
    total = sums[0].astype(jnp.float32)
    for step, copy in zip(order, far):
        copy.wait()
        total = total + landed[step].astype(jnp.float32)
    out[...] = total.astype(out.dtype)


def scatter(parts, partial):
    sides = 2
    height, width = partial.shape[0] // (parts * sides), partial.shape[1]
    blocks = partial.reshape(parts, sides, height, width)
    stack = pltpu.VMEM((parts, height, width), partial.dtype)
    return pl.pallas_call(
        functools.partial(scatter_kernel, parts),
        out_shape=jax.ShapeDtypeStruct((height, width), partial.dtype),
        in_specs=[pl.BlockSpec(memory_space=pltpu.VMEM)],
        out_specs=pl.BlockSpec(memory_space=pltpu.VMEM),
        scratch_shapes=[stack, stack, stack] + [pltpu.SemaphoreType.DMA((parts,))] * 4,
        compiler_params=pltpu.CompilerParams(collective_id=2, has_side_effects=True),
        name="scatter",
    )(blocks)


def shards(
    tokens,
    norm_gain,
    conv_value_weight,
    conv_gate_weight,
    conv_kernel,
    conv_bias,
    channel_gain,
    query_weight,
    key_weight,
    value_weight,
    gate_weight,
    gate_offset,
    start_memory,
    start_norm,
    start_level,
    cell_gain,
    out_conv_weight,
    out_cell_weight,
):
    parts = lax.axis_size(HEAD)
    groups = lax.axis_size(OUTER)
    group = lax.axis_index(OUTER)
    part = lax.axis_index(HEAD)
    key_width = start_norm.shape[2]
    value_width = start_memory.shape[2]
    all_channels = conv_bias.shape[0] * lax.axis_size(TP)
    heads_here = start_level.shape[1]
    channels = conv_bias.shape[0] // parts

    features = tokens.astype(jnp.float32)
    normed = (
        features * lax.rsqrt(jnp.mean(features * features, axis=1, keepdims=True) + EPS) * norm_gain
    ).astype(jnp.bfloat16)

    gate_pre = jnp.dot(normed, gate_weight, preferred_element_type=jnp.float32)
    gate_pre = gate_pre.reshape(gate_pre.shape[0], 2, 2, gate_weight.shape[1] // 4)
    gate_pre = lax.dynamic_slice_in_dim(gate_pre, lax.axis_index(TP) * heads_here, heads_here, 3)
    gate_pre = jnp.transpose(gate_pre, (1, 2, 3, 0)) + gate_offset
    direct = 1 < parts and groups * parts <= 16
    if direct:
        rows, gates, key_value_part, other_part, out_rows = exchange(
            groups,
            parts,
            normed,
            gate_pre,
            key_weight,
            value_weight,
            conv_value_weight,
            conv_gate_weight,
            query_weight,
            out_conv_weight,
            out_cell_weight,
        )
        gates = lax.dynamic_index_in_dim(gates, part, 3, False)
        gates = jnp.transpose(gates, (1, 2, 0, 3)).reshape(gates.shape[1:3] + (-1,))
    else:
        gates = lax.all_gather(gate_pre, (OUTER, HEAD), axis=3, tiled=True)
        gates = lax.dynamic_index_in_dim(gates, part, 2, False)
        rows = lax.all_gather(normed, HEAD, axis=0, tiled=True)
        key_value_part = lax.all_gather(
            spread(by_head((key_weight, value_weight), parts)), OUTER, axis=0, tiled=True
        )
        other_part = lax.all_gather(
            spread(by_head((conv_value_weight, conv_gate_weight, query_weight), parts)),
            OUTER,
            axis=0,
            tiled=True,
        )
        out_rows = spread(by_head((out_conv_weight, out_cell_weight), parts))
    here = rows.shape[0]
    out_part = lax.all_gather(out_rows, OUTER, axis=0, tiled=True)

    key_value = jnp.dot(rows, key_value_part, preferred_element_type=jnp.float32).astype(
        jnp.bfloat16
    )
    others = jnp.dot(rows, other_part, preferred_element_type=jnp.float32).astype(jnp.bfloat16)
    queries = others[:, 2 * channels :]

    gated = (
        others[:, :channels].astype(jnp.float32)
        * jax.nn.sigmoid(others[:, channels : 2 * channels].astype(jnp.float32))
    ).astype(jnp.bfloat16)
    reach = conv_kernel.shape[0] // 2
    up = [(i, i + 1) for i in range(groups - 1)]
    down = [(j, i) for i, j in up]
    before = lax.ppermute(gated[here - reach :], OUTER, up)
    after = lax.ppermute(gated[:reach], OUTER, down)
    key_value, before, after = lax.optimization_barrier((key_value, before, after))
    if direct:
        around = [key_value] + [
            lax.ppermute(key_value, OUTER, [(i, (i + g) % groups) for i in range(groups)])
            for g in range(1, groups)
        ]
        sources = [lax.rem(group + groups - g, groups) for g in range(groups)]
        all_key_value = jnp.concatenate(around, axis=0)
    else:
        all_key_value = lax.all_gather(key_value, OUTER, axis=0, tiled=True)
    padded = jnp.concatenate([before, gated, after], axis=0).astype(jnp.float32)
    taps = own_columns(conv_kernel, parts, part)
    conv_sum = own_columns(conv_bias, parts, part) + sum(
        taps[offset] * padded[offset : offset + here] for offset in range(conv_kernel.shape[0])
    )
    stats = lax.psum(
        jnp.stack([jnp.sum(conv_sum, axis=1), jnp.sum(conv_sum * conv_sum, axis=1)]), (HEAD, TP)
    )
    channel_mean = stats[0] / all_channels
    channel_var = stats[1] / all_channels - channel_mean * channel_mean
    conv_out = jax.nn.silu(
        (conv_sum - channel_mean[:, None])
        * lax.rsqrt(channel_var + EPS)[:, None]
        * own_columns(channel_gain, parts, part)
    ).astype(jnp.bfloat16)

    total = gates.shape[2]
    in_gate = gates[:, 0]
    log_forget = jax.nn.log_sigmoid(gates[:, 1])
    whole = jnp.round(log_forget)
    both = jnp.stack([whole, log_forget - whole])
    both = jnp.stack([both[:, 0], jnp.flip(both[:, 1], axis=1)], axis=1)
    both = running_sum(both)
    passed = jnp.stack([both[:, 0], jnp.flip(both[:, 1], axis=1)], axis=1)
    passed_here = lax.dynamic_slice_in_dim(passed, group * here, here, 2)
    at_column = jnp.arange(total)
    if direct:

        def around_ring(array):
            return jnp.concatenate(
                [lax.dynamic_slice_in_dim(array, g * here, here, array.ndim - 1) for g in sources],
                axis=-1,
            )

        at_column, in_gate, passed = (around_ring(a) for a in (at_column, in_gate, passed))
    at_column = at_column[None, :]
    keys = all_key_value[:, :key_width]
    values = all_key_value[:, key_width:]
    products = lax.dot_general(
        queries, keys, (((1,), (1,)), ((), ())), preferred_element_type=jnp.float32
    ) * (key_width**-0.5)
    at_row = (group * here + jnp.arange(here))[:, None]
    levels = lax.dynamic_index_in_dim(start_level, part, 1, False)
    norms = lax.dynamic_index_in_dim(start_norm, part, 1, False)
    memories = lax.dynamic_index_in_dim(start_memory, part, 1, False)
    wide_queries = queries.astype(jnp.float32)
    scaled = 0.0
    entered = 0.0
    for way in range(2):
        row_whole, row_rest = passed_here[0, way], passed_here[1, way]
        table = (row_whole[:, None] - passed[0, way][None, :]) + (
            row_rest[:, None] + (in_gate[way] - passed[1, way])[None, :]
        )
        seen = at_column <= at_row if way == 0 else at_column >= at_row
        table = jnp.where(seen, table, -jnp.inf)
        start = row_whole + row_rest + levels[way]
        top = jnp.maximum(start, jnp.max(table, axis=1))
        scores = products * jnp.exp(table - top[:, None])
        entry = jnp.exp(start - top)
        denominator = jnp.sum(scores, axis=1) + entry * jnp.sum(
            wide_queries * norms[way][None, :], axis=1
        )
        inverse = 1.0 / jnp.maximum(jnp.abs(denominator), 1.0)
        scaled = scaled + scores * inverse[:, None]
        entered = entered + (entry * inverse)[:, None] * lax.dot_general(
            queries,
            memories[way].astype(jnp.bfloat16),
            (((1,), (1,)), ((), ())),
            preferred_element_type=jnp.float32,
        )
    both_ways = entered + jnp.dot(
        scaled.astype(jnp.bfloat16), values, preferred_element_type=jnp.float32
    )
    both_ways = both_ways * lax.rsqrt(jnp.mean(both_ways * both_ways, axis=1, keepdims=True) + EPS)
    cell_out = (both_ways * own_columns(cell_gain, parts, part)).astype(jnp.bfloat16)

    partial = lax.dot_general(
        jnp.concatenate([conv_out, cell_out], axis=1),
        out_part,
        (((1,), (1,)), ((), ())),
        preferred_element_type=jnp.float32,
    ).astype(jnp.bfloat16)
    if direct and lax.axis_size(TP) == 2:
        return scatter(parts, partial)
    return lax.psum_scatter(partial, (HEAD, TP), scatter_dimension=0, tiled=True)


def solution(mesh):
    split = (OUTER, HEAD)
    in_specs = (
        P(split, None),
        P(),
        P(split, TP),
        P(split, TP),
        P(None, TP),
        P(TP),
        P(TP),
        P(split, TP),
        P(split, TP),
        P(split, TP),
        P(),
        P(None, None, TP, split),
        P(None, TP, None, None),
        P(None, TP, None),
        P(None, TP),
        P(TP),
        P(split, TP),
        P(split, TP),
    )
    out_specs = P((OUTER, HEAD, TP), None)

    def run(*arrays):
        sequence, tensor = mesh.shape["sp"], mesh.shape["tp"]
        heads = arrays[14].shape[1] // tensor
        parts = heads if sequence % heads == 0 else 1
        assert parts == heads
        fine = Mesh(mesh.devices.reshape(sequence // parts, parts, tensor), (OUTER, HEAD, TP))
        return jax.shard_map(
            shards, mesh=fine, in_specs=in_specs, out_specs=out_specs, check_vma=False
        )(*arrays)

    return run
```
